512 devices in a mesh: grp: 2 (over y), dp: 8 (over x), kv: 16 (over z), tp: 2 (over core).
Axes of the slice: x: 8, y: 2, z: 16, core: 2. Of those that a mesh axis runs over, the one named last changes fastest.
The devices are a block of a 8x8x16 slice.
Arguments:
- tokens: bfloat16 [512, 2048], P(('grp', 'dp'), ('kv', 'tp')), parts along dimension 0, may hold values from -24 to 24
- memory: float32 [512, 12, 16384], P(('grp', 'dp', 'kv', 'tp')), parts along dimension 0, may hold values from -3 to 3
- mix_gain: float32 [2048], replicated, may hold values from 0.1 to 1.9
- w_query: bfloat16 [2048, 1536], P(None, ('kv', 'tp')), may hold values from -0.125 to 0.125
- w_key: bfloat16 [2048, 1536], P(None, ('kv', 'tp')), may hold values from -0.125 to 0.125
- w_value: bfloat16 [2048, 1536], P(None, ('kv', 'tp')), may hold values from -0.125 to 0.125
- w_gate: bfloat16 [2048, 1536], P(None, ('kv', 'tp')), may hold values from -0.125 to 0.125
- w_beta: bfloat16 [2048, 12], replicated, may hold values from -0.125 to 0.125
- w_decay: bfloat16 [2048, 12], replicated, may hold values from -0.125 to 0.125
- decay_rate: float32 [12], replicated, may hold values from 0.1 to 3
- decay_bias: float32 [12], replicated, may hold values from -2 to 1
- head_gain: float32 [128], replicated, may hold values from 0.1 to 1.9
- w_out: bfloat16 [1536, 2048], P(None, ('kv', 'tp')), may hold values from -0.15625 to 0.15625
- ffn_gain: float32 [2048], replicated, may hold values from 0.1 to 1.9
- w_up: bfloat16 [2048, 8192], P(None, ('kv', 'tp')), may hold values from -0.125 to 0.125
- w_down: bfloat16 [8192, 2048], P(('kv', 'tp')), may hold values from -0.125 to 0.125
Outputs:
- layer_out: bfloat16 [512, 2048], P(('grp', 'dp'), ('kv', 'tp')), parts along dimension 0
- new_memory: float32 [512, 12, 16384], P(('grp', 'dp', 'kv', 'tp')), parts along dimension 0
The draws below stay inside these ranges and needn't reach their ends.
There are 2 independent parts, one for each index of `grp`. The reference program is written for one: setup_inputs(seed, part) draws one part's arguments, and reference() takes and returns one part's arrays. A program takes and returns all parts, laid end to end along the dimension named above; an argument that names none is the same for every part. Nothing has to cross between parts.
All inputs are finite; a program needn't handle non-finite values.
Results may differ from the reference program's by a relative error of at most 0.02.
Values may be sent and summed in bfloat16 or wider, within the bound.
A program may use at most 64 MiB of HBM per device.

```python
import math
import jax
import jax.numpy as jnp
from jax import lax

D = 2048
HEADS = 12
HEAD_DIM = 128
FF = 8192
BATCH = 256


def draw_tokens(key, part):
    streams = jax.random.split(key, 3)
    trend = jnp.exp(jnp.linspace(math.log(0.5), math.log(1.5), D)).astype(jnp.float32)
    rough = jnp.exp(jax.random.uniform(streams[0], (D,), jnp.float32, -0.5, 0.5))
    row_scale = jnp.exp(jax.random.uniform(streams[1], (BATCH, 1), jnp.float32, -0.7, 0.7))
    base = jax.random.normal(streams[2], (BATCH, D), jnp.float32)
    values = jnp.clip(base * row_scale * trend * rough, -24.0, 24.0)
    return values.astype(jnp.bfloat16)


def strengthened(drawn, stream_key, source, target, shards_of, factor):
    owner, partner = [(jnp.arange(drawn.shape[axis_at]) // (drawn.shape[axis_at] // shards_of)).reshape([-1 if axis == axis_at else 1 for axis in range(drawn.ndim)]) for axis_at in (source, target)]
    chosen = jax.random.permutation(stream_key, shards_of)[partner]
    strong = (owner == chosen) | (owner == (partner + shards_of // 2) % shards_of)
    return jnp.where(strong, factor * drawn, drawn)


def levels(key, dims, shards, low, largest):
    factor_of = 1.0
    for dim, shards_of in shards:
        steps = jax.random.uniform(jax.random.fold_in(jax.random.fold_in(key, 6), dim), (shards_of,), jnp.float32, low / len(shards), largest / len(shards))
        factor_of = factor_of * jnp.repeat(jnp.exp(steps), dims[dim] // shards_of).reshape((-1,) + (1,) * (len(dims) - 1 - dim))
    return factor_of


def gaussian(key, extent, spread, most, shards=(), kind=jnp.bfloat16):
    level = levels(key, extent, shards, -0.22, 0.18) if shards else 1.0
    values = jax.random.normal(key, extent, jnp.float32) * spread * level
    return jnp.minimum(jnp.maximum(values, -most), most).astype(kind)


def noise_with(rng, extent, scale, limit, cuts, heavy, dtype=jnp.bfloat16):
    drawn = scale * jax.random.normal(rng, extent, jnp.float32)
    if cuts:
        drawn = drawn * levels(rng, extent, cuts, -0.22, 0.18)
    return jnp.clip(strengthened(drawn, jax.random.fold_in(rng, 3), *heavy), -limit, limit).astype(dtype)


def setup_inputs(seed: int = 0, part: int = 0) -> dict:
    streams_of = jax.random.split(jax.random.key(seed), 17)
    own_keys = jax.random.split(jax.random.fold_in(streams_of[16], part), 17)
    return {
        "tokens": draw_tokens(jax.random.fold_in(jax.random.fold_in(streams_of[16], part), 71), part),
        "memory": gaussian(own_keys[1], (BATCH, HEADS, HEAD_DIM * HEAD_DIM), 0.5, 3.0, ((0, 256),), jnp.float32),
        "mix_gain": jnp.clip(1.0 + 0.18 * jax.random.normal(streams_of[2], (D,), jnp.float32), 0.1, 1.9),
        "w_query": gaussian(streams_of[3], (D, HEADS * HEAD_DIM), D ** -0.5, 0.125, ((1, 32),)),
        "w_key": gaussian(streams_of[4], (D, HEADS * HEAD_DIM), D ** -0.5, 0.125, ((1, 32),)),
        "w_value": gaussian(streams_of[5], (D, HEADS * HEAD_DIM), D ** -0.5, 0.125, ((1, 32),)),
        "w_gate": gaussian(streams_of[6], (D, HEADS * HEAD_DIM), D ** -0.5, 0.125, ((1, 32),)),
        "w_beta": gaussian(streams_of[7], (D, HEADS), D ** -0.5, 0.125),
        "w_decay": gaussian(streams_of[8], (D, HEADS), D ** -0.5, 0.125),
        "decay_rate": jnp.clip(jnp.exp(jax.random.uniform(streams_of[9], (HEADS,), jnp.float32, math.log(0.1), math.log(3.0))), 0.1, 3.0),
        "decay_bias": jnp.clip(jax.random.uniform(streams_of[10], (HEADS,), jnp.float32, -2.0, 1.0), -2.0, 1.0),
        "head_gain": jnp.clip(1.0 + 0.18 * jax.random.normal(streams_of[11], (HEAD_DIM,), jnp.float32), 0.1, 1.9),
        "w_out": gaussian(streams_of[12], (HEADS * HEAD_DIM, D), (HEADS * HEAD_DIM) ** -0.5, 0.15625, ((1, 32),)),
        "ffn_gain": jnp.clip(1.0 + 0.18 * jax.random.normal(streams_of[13], (D,), jnp.float32), 0.1, 1.9),
        "w_up": gaussian(streams_of[14], (D, FF), D ** -0.5, 0.125, ((1, 32),)),
        "w_down": noise_with(streams_of[15], (FF, D), FF ** -0.5, 0.125, ((0, 32),), (0, 1, 32, 2.75)),
    }


epsilon = 1e-06

def delta_step(queries, keys_in, values, gates, strength, log_decay, memory, head_gain):
    count = queries.shape[0]
    heads = strength.shape[1]
    size = head_gain.shape[0]
    highest = lax.Precision.HIGHEST
    query_wide = queries.astype(jnp.float32).reshape(count, heads, size)
    key_wide = keys_in.astype(jnp.float32).reshape(count, heads, size)
    value_wide = values.astype(jnp.float32).reshape(count, heads, size)
    gate_wide = gates.astype(jnp.float32).reshape(count, heads, size)
    unit_key = key_wide * lax.rsqrt(lax.optimization_barrier(jnp.sum(key_wide * key_wide, axis=-1, keepdims=True)) + epsilon)
    matrix = memory.reshape(count, heads, size, size)
    recall = jnp.einsum('bhk,bhkv->bhv', unit_key, matrix, precision=highest)
    retain = jnp.exp(log_decay)[:, :, None, None]
    scaled = strength[:, :, None]
    erased = matrix - jnp.einsum('bhk,bhv->bhkv', unit_key, scaled * recall, precision=highest)
    written = jnp.einsum('bhk,bhv->bhkv', unit_key, scaled * value_wide, precision=highest)
    updated = retain * erased + written
    readout = jnp.einsum('bhk,bhkv->bhv', query_wide, updated, precision=highest)
    normed = readout * lax.rsqrt(lax.optimization_barrier(jnp.mean(readout * readout, axis=-1, keepdims=True)) + epsilon)
    normed = normed * head_gain * jax.nn.silu(gate_wide)
    return (updated.reshape(count, heads, size * size), normed.reshape(count, heads * size).astype(jnp.bfloat16))

def reference(tokens, memory, mix_gain, w_query, w_key, w_value, w_gate, w_beta, w_decay, decay_rate, decay_bias, head_gain, w_out, ffn_gain, w_up, w_down):
    width = tokens.shape[1]
    wide = tokens.astype(jnp.float32)
    scale_in = lax.rsqrt(lax.optimization_barrier(jnp.sum(wide * wide, axis=1)) / width + epsilon)[:, None]
    lifted_in = (wide * mix_gain).astype(jnp.bfloat16)

    def project(weight):
        return jnp.dot(lifted_in, weight, preferred_element_type=jnp.float32) * scale_in
    queries = project(w_query).astype(jnp.bfloat16)
    keys_in = project(w_key).astype(jnp.bfloat16)
    values = project(w_value).astype(jnp.bfloat16)
    gates = project(w_gate).astype(jnp.bfloat16)
    strength = jax.nn.sigmoid(project(w_beta))
    log_decay = -decay_rate * jax.nn.softplus(project(w_decay) + decay_bias)
    updated, mixed = delta_step(queries, keys_in, values, gates, strength, log_decay, memory, head_gain)
    branch = jnp.dot(mixed, w_out, preferred_element_type=jnp.float32)
    middle = (wide + branch).astype(jnp.bfloat16)
    middle_wide = middle.astype(jnp.float32)
    scale_mid = lax.rsqrt(lax.optimization_barrier(jnp.sum(middle_wide * middle_wide, axis=1)) / width + epsilon)[:, None]
    lifted_mid = (middle_wide * ffn_gain).astype(jnp.bfloat16)
    hidden = jnp.square(jax.nn.relu(jnp.dot(lifted_mid, w_up, preferred_element_type=jnp.float32) * scale_mid))
    hidden = hidden.astype(jnp.bfloat16)
    layer_out = (middle_wide + jnp.dot(hidden, w_down, preferred_element_type=jnp.float32)).astype(jnp.bfloat16)
    return (layer_out, updated)
```

```python
import functools
import jax
import jax.numpy as jnp
from jax import lax
from jax.experimental import pallas as pl
from jax.experimental.pallas import tpu as pltpu
from jax.sharding import PartitionSpec as P

epsilon = 1e-06
f32 = jnp.float32
bf16 = jnp.bfloat16
MESH = pl.DeviceIdType.MESH


def far_first(chips):
    return sorted(range(1, chips), key=lambda d: -min(d, chips - d))


def layer_kernel(
    tokens_hbm, memory_hbm, mix_gain_hbm, wq_hbm, wk_hbm, wv_hbm, wg_hbm, wbeta_hbm, wdecay_hbm,
    rate_hbm, bias_hbm, head_gain_hbm, wout_hbm, ffn_gain_hbm, wup_hbm, wdown_hbm,
    out_ref, new_memory_hbm,
    wproj, wsmall, wout, wup, wdown,
    state, state_out, tok, mix_gain, ffn_gain, rate, bias, head_gain,
    send1, buf1, send2, buf2, send3, buf3, send4, buf4, send5, buf5, midx,
    tokf, rawx, lift, scr_t, scr_a, scr_b, scr_c, scr_o,
    load_sem, wload_sem, wsend_sem, wrecv_sem, send_sem, recv_sem,
):
    chips = lax.axis_size("kv")
    cores = lax.axis_size("tp")
    z = lax.axis_index("kv")
    c = lax.axis_index("tp")
    other = 1 - c
    me = z * cores + c
    heads, size = 12, 128

    def chip_at(d):
        return lax.rem(z + d, chips)

    barrier = pltpu.get_barrier_semaphore()
    peers = [(d, k) for d in far_first(chips) for k in (0, 1)]
    for d, k in peers:
        pl.semaphore_signal(
            barrier, inc=1, device_id={"kv": chip_at(d), "tp": lax.rem(c + k, cores)},
            device_id_type=MESH,
        )
    pl.semaphore_signal(barrier, inc=1, device_id={"kv": z, "tp": other}, device_id_type=MESH)

    tok_copy = pltpu.make_async_copy(tokens_hbm, tok, load_sem.at[0])
    tok_copy.start()
    small = [
        pltpu.make_async_copy(src, dst, load_sem.at[1 + i])
        for i, (src, dst) in enumerate(
            (
                (mix_gain_hbm, mix_gain), (ffn_gain_hbm, ffn_gain), (rate_hbm, rate),
                (bias_hbm, bias), (head_gain_hbm, head_gain), (wbeta_hbm, wsmall.at[0]),
                (wdecay_hbm, wsmall.at[1]),
            )
        )
    ]
    for copy in small:
        copy.start()
    narrow, depth = wq_hbm.shape
    width = cores * narrow

    def rows_of(ref, start, count):
        return ref.at[pl.ds(pl.multiple_of(start + c * count, 16), count)]

    shared = [
        (wq_hbm, rows_of(wproj, 0, narrow)), (wk_hbm, rows_of(wproj, size, narrow)),
        (wv_hbm, rows_of(wproj, 2 * size, narrow)), (wg_hbm, rows_of(wproj, 3 * size, narrow)),
        (wout_hbm, rows_of(wout, 0, wout_hbm.shape[0])), (wup_hbm, wup.at[c]),
        (wdown_hbm, wdown.at[c]),
    ]
    own_weights = [
        pltpu.make_async_copy(src, dst, wload_sem.at[i])
        for i, (src, dst) in enumerate(shared)
    ]
    for copy in own_weights:
        copy.start()
    state_copy = pltpu.make_async_copy(memory_hbm, state, load_sem.at[8])
    state_copy.start()

    tok_copy.wait()
    tokf[:, 0 : tok.shape[1]] = tok[...].astype(f32)
    half_rows = chips // 2
    for k in range(2):
        part = tokf[pl.ds(k, chips, stride=2), :]
        cols = tok.shape[1]
        send1[k] = jnp.concatenate(
            [part[:half_rows, :cols], part[half_rows:, :cols]], axis=1
        ).astype(bf16)
    buf1[me] = send1[c]

    pl.semaphore_wait(barrier, len(peers) + 1)

    def send(src, dst, phase, d, core):
        pltpu.make_async_remote_copy(
            src_ref=src, dst_ref=dst, send_sem=send_sem.at[phase], recv_sem=recv_sem.at[phase],
            device_id={"kv": chip_at(d), "tp": core}, device_id_type=MESH,
        ).start()

    for d in far_first(chips):
        for k in range(2):
            core = lax.rem(c + k, cores)
            send(send1.at[core], buf1.at[me], 0, d, core)
    send(send1.at[other], buf1.at[me], 0, 0, other)

    swap = []
    for i, (src, dst) in enumerate(shared):
        copy = pltpu.make_async_remote_copy(
            src_ref=src, dst_ref=dst, send_sem=wsend_sem.at[i], recv_sem=wrecv_sem.at[i],
            device_id={"kv": z, "tp": other}, device_id_type=MESH,
        )
        copy.start()
        swap.append(copy)

    for copy in small:
        copy.wait()
    spare = size - width
    for x in range(4):
        if x < 2:
            rest = jnp.zeros((spare - heads, depth), bf16)
            rest = jnp.concatenate([wsmall[x].astype(f32), rest.astype(f32)], axis=0).astype(bf16)
        else:
            rest = jnp.zeros((spare, depth), bf16)
        wproj[x * size + width : (x + 1) * size, :] = rest
    for i in range(5):
        own_weights[i].wait()
        swap[i].wait_recv()

    def rows_dot(a, b):
        return lax.dot_general(a, b, (((1,), (1,)), ((), ())), preferred_element_type=f32)

    def arrived(buf, count, phase):
        pltpu.make_async_copy(
            buf.at[pl.ds(0, count)], buf.at[pl.ds(0, count)], recv_sem.at[phase]
        ).wait()

    def sent(buf, count, phase):
        pltpu.make_async_copy(
            buf.at[pl.ds(0, count)], buf.at[pl.ds(0, count)], send_sem.at[phase]
        ).wait()

    arrived(buf1, 2 * chips - 1, 0)
    squares = jnp.zeros((chips, size), f32)
    cols = size // 2
    for j in range(chips):
        even = buf1[2 * j].astype(f32)
        odd = buf1[2 * j + 1].astype(f32)
        top = jnp.concatenate([even[:, :cols], odd[:, :cols]], axis=1)
        low = jnp.concatenate([even[:, cols:], odd[:, cols:]], axis=1)
        x = jnp.concatenate([top, low], axis=0)
        rawx[j] = x
        squares += x * x
        lift[:, j * size : (j + 1) * size] = (x * mix_gain[j : j + 1, :]).astype(bf16)
    scale_in = lax.rsqrt(jnp.sum(squares, axis=1, keepdims=True) / depth + epsilon)
    total = rows_dot(lift[...], wproj[...]) * scale_in

    offset = lax.rem(z * width, size)
    scr_a[...] = jnp.zeros_like(scr_a)
    for x in range(4):
        piece = total[:, x * size : (x + 1) * size]
        if x < 2:
            scr_t[x] = piece
        scr_a[pl.ds(x, chips, stride=8), :] = pltpu.roll(
            piece.astype(bf16).astype(f32), offset, axis=1
        )
    send2[...] = scr_a[...].reshape(chips, 8, size).astype(bf16)
    for d in far_first(chips):
        send(send2.at[chip_at(d)], buf2.at[z], 1, d, c)
    buf2[z] = send2[z]

    lane = lax.broadcasted_iota(jnp.int32, (heads, size), 1)
    head = lax.broadcasted_iota(jnp.int32, (heads, size), 0)
    chosen = lane == head + width

    def own_column(x):
        row = jnp.broadcast_to(scr_t[x, pl.ds(z, 1), :], (heads, size))
        return jnp.sum(jnp.where(chosen, row, 0.0), axis=1, keepdims=True)

    def as_column(row):
        diagonal = lane[:, :heads] == head[:, :heads]
        spread = jnp.where(diagonal, jnp.broadcast_to(row, (heads, heads)), 0.0)
        return jnp.sum(spread, axis=1, keepdims=True)

    strength = jax.nn.sigmoid(own_column(0))
    rate_col = as_column(rate[...])
    bias_col = as_column(bias[...])
    lifted = own_column(1) + bias_col
    softplus = jnp.maximum(lifted, 0.0) + jnp.log(1.0 + jnp.exp(-jnp.abs(lifted)))
    retain = jnp.exp(-rate_col * softplus)
    state_copy.wait()

    arrived(buf2, chips - 1, 1)
    lane8 = lax.broadcasted_iota(jnp.int32, (8, size), 1)
    for h in range(heads):
        first = (h * size) // width
        tile = buf2[first].astype(f32)
        end = (first + 1) * width - h * size
        nxt = buf2[first + 1].astype(f32)
        scr_b[8 * h : 8 * h + 8, :] = jnp.where(lane8 < end, tile, nxt)
    query = scr_b[pl.ds(0, heads, stride=8), :]
    key = scr_b[pl.ds(1, heads, stride=8), :]
    value = scr_b[pl.ds(2, heads, stride=8), :]
    gate = scr_b[pl.ds(3, heads, stride=8), :]
    unit = key * lax.rsqrt(jnp.sum(key * key, axis=1, keepdims=True) + epsilon)

    def columns(rows):
        pad = jnp.zeros((16 - heads, size), f32)
        return jnp.concatenate([rows, pad], axis=0).T

    unit_cols = columns(unit)
    query_cols = columns(query)
    recall, asked = [], []
    for h in range(heads):
        s = state[h]
        recall.append(jnp.sum(s * unit_cols[:, h : h + 1], axis=0, keepdims=True))
        asked.append(jnp.sum(s * query_cols[:, h : h + 1], axis=0, keepdims=True))
    recall = jnp.concatenate(recall, axis=0)
    asked = jnp.concatenate(asked, axis=0)
    write = strength * (value - retain * recall)
    readout = retain * asked + jnp.sum(unit * query, axis=1, keepdims=True) * write
    normed = readout * lax.rsqrt(jnp.mean(readout * readout, axis=1, keepdims=True) + epsilon)
    normed = normed * head_gain[...] * (gate * jax.nn.sigmoid(gate))

    send3[0] = jnp.concatenate([normed, jnp.zeros((16 - heads, size), f32)], axis=0).astype(bf16)
    for d in far_first(chips):
        send(send3.at[0], buf3.at[z], 2, d, c)
    buf3[z] = send3[0]

    for h in range(heads):
        state_out[h] = (
            retain[h : h + 1, :] * state[h] + unit_cols[:, h : h + 1] * write[h : h + 1, :]
        )
    store_copy = pltpu.make_async_copy(state_out, new_memory_hbm, load_sem.at[9])
    store_copy.start()

    arrived(buf3, chips - 1, 2)
    for j in range(chips):
        scr_c[16 * j : 16 * j + 16, :] = buf3[j].astype(f32)
    mixed = jnp.concatenate(
        [scr_c[pl.ds(h, chips, stride=16), :].astype(bf16) for h in range(heads)], axis=1
    )
    branch = rows_dot(mixed, wout[...])
    middle = (rawx[z] + branch).astype(bf16)

    send4[0] = middle
    for d in far_first(chips):
        send(send4.at[0], buf4.at[z], 3, d, c)
    buf4[z] = middle
    middle_wide = middle.astype(f32)

    def split(tile):
        top, low = tile[:half_rows], tile[half_rows:]
        return (
            jnp.concatenate([top[:, :cols], low[:, :cols]], axis=1),
            jnp.concatenate([top[:, cols:], low[:, cols:]], axis=1),
        )

    for k, part in enumerate(split(middle_wide)):
        send4[1, 8 * k : 8 * k + 8] = part.astype(bf16)
        scr_o[8 * k : 8 * k + 8, :] = part
    mid_send = pltpu.make_async_remote_copy(
        src_ref=send4.at[1], dst_ref=midx, send_sem=send_sem.at[5], recv_sem=recv_sem.at[5],
        device_id={"kv": z, "tp": other}, device_id_type=MESH,
    )
    mid_send.start()
    for i in (5, 6):
        own_weights[i].wait()
        swap[i].wait_recv()
    mid_send.wait_recv()

    arrived(buf4, chips - 1, 3)
    squares = jnp.zeros((chips, size), f32)
    for j in range(chips):
        x = buf4[j].astype(f32)
        squares += x * x
        lift[:, j * size : (j + 1) * size] = (x * ffn_gain[j : j + 1, :]).astype(bf16)
    scale_mid = lax.rsqrt(jnp.sum(squares, axis=1, keepdims=True) / depth + epsilon)
    terms = None
    for k in range(2):
        raised = jnp.dot(lift[...], wup[k], preferred_element_type=f32)
        hidden = jnp.square(jnp.maximum(raised * scale_mid, 0.0)).astype(bf16)
        term = jnp.dot(hidden, wdown[k], preferred_element_type=f32)
        terms = term if terms is None else terms + term

    for j in range(chips):
        for k, part in enumerate(split(terms[:, j * size : (j + 1) * size])):
            send5[2 * j + k] = part.astype(bf16)
    for d in far_first(chips):
        for k in range(2):
            core = lax.rem(c + k, cores)
            send(send5.at[chip_at(d) * cores + core], buf5.at[me], 4, d, core)
    send(send5.at[z * cores + other], buf5.at[me], 4, 0, other)
    buf5[me] = send5[me]
    arrived(buf5, 2 * chips - 1, 4)
    mine = scr_o[pl.ds(pl.multiple_of(c * 8, 8), 8), :]
    halves = midx[...].astype(f32)
    theirs = jnp.where(c == 0, halves[0:8], halves[8:16])
    for k in range(2):
        down = buf5[k].astype(f32)
        for j in range(1, chips):
            down += buf5[2 * j + k].astype(f32)
        down += jnp.where(c == k, mine, theirs)
        tokf[pl.ds(k, half_rows, stride=2), :] = down
        tokf[pl.ds(chips + k, half_rows, stride=2), 0:cols] = down[:, cols:]
    out_ref[...] = tokf[:, 0:cols].astype(bf16)

    sent(buf1, 2 * chips - 1, 0)
    sent(buf2, chips - 1, 1)
    sent(buf3, chips - 1, 2)
    sent(buf4, chips - 1, 3)
    sent(buf5, 2 * chips - 1, 4)
    mid_send.wait_send()
    for copy in swap:
        copy.wait_send()
    store_copy.wait()


def per_device(
    tokens, memory, mix_gain, w_query, w_key, w_value, w_gate, w_beta, w_decay,
    decay_rate, decay_bias, head_gain, w_out, ffn_gain, w_up, w_down,
):
    chips = lax.axis_size("kv")
    rows, columns = tokens.shape
    depth = w_query.shape[0]
    heads = memory.shape[1]
    size = head_gain.shape[0]

    hbm = pl.BlockSpec(memory_space=pl.ANY)
    V = pltpu.VMEM
    DMA = pltpu.SemaphoreType.DMA
    state_shape = (heads, size, size)
    layer_out, new_memory = pl.pallas_call(
        layer_kernel,
        out_shape=(
            jax.ShapeDtypeStruct((rows, columns), bf16),
            jax.ShapeDtypeStruct(state_shape, f32),
        ),
        in_specs=[hbm] * 16,
        out_specs=(pl.BlockSpec(memory_space=pltpu.VMEM), hbm),
        scratch_shapes=[
            V((4 * size, depth), bf16), V((2, heads, depth), bf16),
            V((2 * columns, w_out.shape[0]), bf16), V((2,) + w_up.shape, bf16),
            V((2,) + w_down.shape, bf16),
            V(state_shape, f32), V(state_shape, f32), V(tokens.shape, bf16),
            V((depth // size, size), f32), V((depth // size, size), f32),
            V((1, heads), f32), V((1, heads), f32), V((1, size), f32),
            V((2, 8, size), bf16), V((2 * chips, 8, size), bf16),
            V((chips, 8, size), bf16), V((chips, 8, size), bf16),
            V((1, 16, size), bf16), V((chips, 16, size), bf16),
            V((2, 16, size), bf16), V((chips, 16, size), bf16),
            V((2 * chips, 8, size), bf16), V((2 * chips, 8, size), bf16),
            V((16, size), bf16),
            V((rows, size), f32), V((chips, chips, size), f32), V((chips, depth), bf16),
            V((2, chips, size), f32), V((chips * 8, size), f32), V((heads * 8, size), f32),
            V((chips * 16, size), f32), V((16, size), f32),
            DMA((10,)), DMA((7,)), DMA((7,)), DMA((7,)), DMA((6,)), DMA((6,)),
        ],
        compiler_params=pltpu.CompilerParams(collective_id=0, has_side_effects=True),
    )(
        tokens, memory.reshape(state_shape), mix_gain.reshape(-1, size), w_query.T, w_key.T,
        w_value.T, w_gate.T, w_beta.T, w_decay.T, decay_rate.reshape(1, heads),
        decay_bias.reshape(1, heads), head_gain.reshape(1, size), w_out.T,
        ffn_gain.reshape(-1, size), w_up, w_down,
    )
    return layer_out, new_memory.reshape(memory.shape)


def solution(mesh):
    lanes = ("kv", "tp")
    placed = (
        P(("grp", "dp"), lanes), P(("grp", "dp") + lanes, None, None), P(),
        P(None, lanes), P(None, lanes), P(None, lanes), P(None, lanes),
        P(), P(), P(), P(), P(), P(None, lanes), P(), P(None, lanes), P(lanes, None),
    )
    return jax.shard_map(
        per_device, mesh=mesh, in_specs=placed,
        out_specs=(P(("grp", "dp"), lanes), P(("grp", "dp") + lanes, None, None)),
        check_vma=False,
    )
```
